32 devices in a mesh: fs: 8 (over z, y), tp: 4 (over x, core).
Axes of the slice: x: 2, y: 2, z: 4, core: 2. Of those that a mesh axis runs over, the one named last changes fastest.
Arguments:
- inputs: bfloat16 [9216, 2048], P('fs'), may hold values from -6 to 6
- gate_cot: bfloat16 [9216, 4096], P('fs', 'tp'), may hold values from -0.0546875 to 0.0546875
- state_cot: bfloat16 [9216, 1024], P('fs', 'tp'), may hold values from -0.0546875 to 0.0546875
- gate_weight: float32 [2048, 4096], P('fs', 'tp'), may hold values from -0.75 to 0.75
- state_weight: float32 [2048, 1024], P('fs', 'tp'), may hold values from -0.75 to 0.75
- gate_factor: bfloat16 [2048, 256], P('fs'), may hold values from -0.375 to 0.375
- state_factor: bfloat16 [2048, 256], P('fs'), may hold values from -0.375 to 0.375
- gate_first: float32 [256, 4096], P('fs', 'tp'), may hold values from -6 to 6
- gate_second: float32 [256, 4096], P('fs', 'tp'), may hold values from 0.3 to 3
- state_first: float32 [256, 1024], P('fs', 'tp'), may hold values from -6 to 6
- state_second: float32 [256, 1024], P('fs', 'tp'), may hold values from 0.3 to 3
Outputs:
- new_gate_weight: float32 [2048, 4096], P('fs', 'tp')
- new_state_weight: float32 [2048, 1024], P('fs', 'tp')
- gate_copy: bfloat16 [2048, 4096], P(None, 'tp')
- state_copy: bfloat16 [2048, 1024], P(None, 'tp')
- new_gate_first: float32 [256, 4096], P('fs', 'tp')
- new_gate_second: float32 [256, 4096], P('fs', 'tp')
- new_state_first: float32 [256, 1024], P('fs', 'tp')
- new_state_second: float32 [256, 1024], P('fs', 'tp')
The draws below stay inside these ranges and needn't reach their ends.
All inputs are finite; a program needn't handle non-finite values.
Results may differ from the reference program's by a relative error of at most 0.004.
Values may be sent and summed in bfloat16 or wider, within the bound.
A program may use at most 128 MiB of HBM per device.

```python
import math
import jax
import jax.numpy as jnp
from jax import lax

D = 2048
DI = 4096
BW = 1024
RANK = 256
TOK_DEV = 1152
TOKENS = 9216
N_FS = 8


def block_levels(rng, shape, split, low, largest):
    level = 1.0
    for position, parts in split:
        heights = jax.random.uniform(jax.random.fold_in(jax.random.fold_in(rng, 6), position), (parts,), jnp.float32, low / len(split), largest / len(split))
        level = level * jnp.repeat(jnp.exp(heights), shape[position] // parts).reshape((-1,) + (1,) * (len(shape) - 1 - position))
    return level


def centred(own_key, dims, width, limit, shards=(), kind=jnp.bfloat16):
    result = jax.random.normal(own_key, dims, jnp.float32) * width
    if len(shards) > 0:
        result = block_levels(own_key, dims, shards, -0.22, 0.18) * result
    return jnp.clip(result, min=-limit, max=limit).astype(kind)


def setup_inputs(seed: int = 0) -> dict:
    arg_keys = jax.random.split(jax.random.key(seed), 12)
    inputs = centred(arg_keys[0], (TOKENS, D), 1.0, 6.0, ((0, 8),))
    gate_cot = centred(arg_keys[1], (TOKENS, DI), (0.35 / (TOK_DEV * N_FS) ** 0.5), 0.0546875, ((0, 8), (1, 4)))
    state_cot = centred(arg_keys[2], (TOKENS, BW), (0.35 / (TOK_DEV * N_FS) ** 0.5), 0.0546875, ((0, 8), (1, 4)))
    gate_weight = centred(arg_keys[3], (D, DI), 0.05, 0.75, ((0, 8), (1, 4)), jnp.float32)
    state_weight = centred(arg_keys[4], (D, BW), 0.05, 0.75, ((0, 8), (1, 4)), jnp.float32)
    gate_factor = centred(arg_keys[5], (D, RANK), RANK ** -0.5, 0.375, ((0, 8),))
    state_factor = centred(arg_keys[6], (D, RANK), RANK ** -0.5, 0.375, ((0, 8),))
    gate_first = centred(arg_keys[7], (RANK, DI), 1.0, 6.0, ((0, 8), (1, 4)), jnp.float32)
    gate_second = jnp.clip(jnp.exp(math.log(3.0) - 2.3025851 * jax.random.uniform(arg_keys[8], (RANK, DI), jnp.float32) ** block_levels(arg_keys[8], (RANK, DI), ((0, 8), (1, 4)), -0.2, 0.2)), 0.3, 3.0)
    state_first = centred(arg_keys[9], (RANK, BW), 1.0, 6.0, ((0, 8), (1, 4)), jnp.float32)
    state_second = jnp.clip(jnp.exp(math.log(3.0) - 2.3025851 * jax.random.uniform(arg_keys[10], (RANK, BW), jnp.float32) ** block_levels(arg_keys[10], (RANK, BW), ((0, 8), (1, 4)), -0.2, 0.2)), 0.3, 3.0)
    return dict(inputs=inputs, gate_cot=gate_cot, state_cot=state_cot, gate_weight=gate_weight, state_weight=state_weight, gate_factor=gate_factor, state_factor=state_factor, gate_first=gate_first, gate_second=gate_second, state_first=state_first, state_second=state_second)


def update_one(inputs, cot, weight, factor, first, second):
    inputs_wide = inputs.astype(jnp.float32)
    factor_wide = factor.astype(jnp.float32)
    lifted = jnp.dot(inputs_wide, factor_wide, precision=lax.Precision.HIGHEST)
    proj = jnp.dot(lifted.T, cot.astype(jnp.float32), precision=lax.Precision.HIGHEST)
    first_new = 0.8 * first + 0.2 * proj
    second_new = 0.9 * second + 0.1 * proj * proj
    direction = (first_new / jnp.sqrt(second_new)).astype(jnp.bfloat16)
    full = jnp.dot(factor_wide, direction.astype(jnp.float32), precision=lax.Precision.HIGHEST)
    scale = 0.02 / jnp.sqrt(jnp.mean(full * full) + 0.25)
    updated = weight - scale * full
    return (updated, updated.astype(jnp.bfloat16), first_new, second_new)

def reference(inputs, gate_cot, state_cot, gate_weight, state_weight, gate_factor, state_factor, gate_first, gate_second, state_first, state_second):
    gate_new, gate_copy, gate_first_new, gate_second_new = update_one(inputs, gate_cot, gate_weight, gate_factor, gate_first, gate_second)
    state_new, state_copy, state_first_new, state_second_new = update_one(inputs, state_cot, state_weight, state_factor, state_first, state_second)
    return (gate_new, state_new, gate_copy, state_copy, gate_first_new, gate_second_new, state_first_new, state_second_new)
```

```python
import functools

import jax
import jax.numpy as jnp
from jax import lax
from jax.experimental import pallas as pl
from jax.experimental.pallas import tpu as pltpu
from jax.sharding import PartitionSpec as P

MESH = pl.DeviceIdType.MESH
BF16 = jnp.bfloat16
F32 = jnp.float32


def over_rows(a, b):
    return lax.dot_general(a, b, (((0,), (0,)), ((), ())), preferred_element_type=F32)


def split(a):
    upper = a.astype(BF16)
    return upper, (a - upper.astype(F32)).astype(BF16)


def exchange_kernel(
    n, tp, tiles, sizes,
    x_hbm, gcot_hbm, scot_hbm, gw_hbm, sw_hbm, gf_hbm, sf_hbm, gfirst_hbm, gsecond_hbm, sfirst_hbm, ssecond_hbm,
    wout, wnew, fnew, snew,
    wg, f_all, dirs, x, gcot, scot, wide, wown, first, second, acc, send_y, recv_y, send_z, recv_z, sums, sums_in,
    load,
    f_send, f_recv, fx_send, fx_recv, fc_send, fc_recv, fd_send, fd_recv,
    ry_send, ry_recv, rz_send, rz_recv, d_send, d_recv, s_send, s_recv, w_send, w_recv,
):
    me = lax.axis_index("fs")
    t = lax.axis_index("tp")
    rows, rank = gf_hbm.shape
    gc = gcot.shape[1]
    sc = scot.shape[1]
    r = first.shape[0]
    q = rows // tp
    half = rows // 2
    depth = n // 2
    z, y = me // 2, me % 2
    partner = 2 * z + 1 - y

    sources = [
        (gf_hbm, f_all.at[me, :, pl.ds(0, rank)]),
        (sf_hbm, f_all.at[me, :, pl.ds(rank, rank)]),
        (gw_hbm, wide.at[:, pl.ds(0, gc)]),
        (sw_hbm, wide.at[:, pl.ds(gc, sc)]),
        (x_hbm, x),
        (gcot_hbm, gcot),
        (scot_hbm, scot),
        (gfirst_hbm, first.at[:, pl.ds(0, gc)]),
        (sfirst_hbm, first.at[:, pl.ds(gc, sc)]),
        (gsecond_hbm, second.at[:, pl.ds(0, gc)]),
        (ssecond_hbm, second.at[:, pl.ds(gc, sc)]),
    ]
    loads = [pltpu.make_async_copy(src, dst, load.at[k]) for k, (src, dst) in enumerate(sources)]
    for c in loads:
        c.start()

    def along_z(k):
        return 2 * ((z + depth + k) % depth) + y

    barrier = pltpu.get_barrier_semaphore()
    pl.semaphore_signal(barrier, inc=1, device_id=(partner, t), device_id_type=MESH)
    for k in range(1, depth):
        pl.semaphore_signal(barrier, inc=1, device_id=(along_z(k), t), device_id_type=MESH)
    for d in range(1, tp):
        pl.semaphore_signal(barrier, inc=1, device_id=(me, (t + d) % tp), device_id_type=MESH)
    pl.semaphore_wait(barrier, depth + tp - 1)

    def remote(src, dst, ss, rs, dev):
        return pltpu.make_async_remote_copy(
            src_ref=src, dst_ref=dst, send_sem=ss, recv_sem=rs, device_id=dev, device_id_type=MESH
        )

    core_peer = t + 1 - 2 * (t % 2)
    x_peer = (t + 2) % tp

    def source_block(j):
        k = j % depth
        return 2 * ((z + depth - k) % depth) + (y if j < depth else 1 - y)

    def quarter(block, which):
        return f_all.at[block, pl.ds(which * q, q), :]

    def first_leg(view, send, recv):
        copies = {}
        for j in sorted(range(1, depth), key=lambda k: -min(k, depth - k)) + [depth]:
            dev = partner if j == depth else along_z(j)
            copies[j] = remote(view(me), view(me), send.at[j], recv.at[j], (dev, t))
            copies[j].start()
        return copies

    def pass_over(copies, view, send, recv, k):
        b = source_block(k)
        copies[depth + k] = remote(
            view(b), view(b), send.at[depth + k], recv.at[depth + k], (partner, t)
        )
        copies[depth + k].start()

    loads[0].wait()
    loads[1].wait()
    mine = lambda b: quarter(b, t)
    f_copies = first_leg(mine, f_send, f_recv)

    loads[2].wait()
    loads[3].wait()
    wown[...] = wide[...].astype(BF16)

    shares = {}

    def share(j):
        src = quarter(source_block(j), t)
        cx = remote(src, src, fx_send.at[j], fx_recv.at[j], (me, x_peer))
        cx.start()
        cc = remote(src, src, fc_send.at[j], fc_recv.at[j], (me, core_peer))
        cc.start()
        shares[j] = [cx, cc]

    order = sorted(range(1, depth), key=lambda k: min(k, depth - k))
    for k in order:
        f_copies[k].wait_recv()
        pass_over(f_copies, mine, f_send, f_recv, k)
        share(k)

    pos = z + y * (n - 1 - 2 * z)

    def at_pos(p):
        p = (p + n) % n
        far = p // (n // 2)
        return 2 * p * (1 - far) + far * (2 * (n - 1 - p) + 1)

    right, left = at_pos(pos + 1), at_pos(pos - 1)
    steps = n // 2

    def w_copy(way, s, h):
        block = at_pos(pos - s) if way == 0 else at_pos(pos + s)
        dst = wg.at[block, pl.ds(h * half, half), :]
        src = wown.at[pl.ds(h * half, half), :] if s == 0 else dst
        return remote(
            src, dst, w_send.at[way, s, h], w_recv.at[way, s, h], (right if way == 0 else left, t)
        )

    def halves(way, s):
        return (0, 1) if s < steps - 1 else (way,)

    w_copies = {}

    def ring_step(s, parts=(0, 1)):
        for k in parts:
            for way in (0, 1):
                h = k if way == 0 else 1 - k
                if s > 0:
                    w_copies[way, s - 1, h].wait_recv()
                if h in halves(way, s):
                    w_copies[way, s, h] = w_copy(way, s, h)
                    w_copies[way, s, h].start()

    ring_step(0)

    for k in [0] + order:
        f_copies[depth + k].wait_recv()
        share(depth + k)
    for j, pair in shares.items():
        pair[0].wait_recv()
        src = quarter(source_block(j), x_peer)
        cd = remote(src, src, fd_send.at[j], fd_recv.at[j], (me, core_peer))
        cd.start()
        pair.append(cd)
    for cx, cc, cd in shares.values():
        cc.wait_recv()
        cd.wait_recv()

    ring_step(1, (0,))
    for k in (4, 5, 6):
        loads[k].wait()
    factor = f_all.reshape(n * rows, 2 * rank)
    step = x.shape[0] // tiles
    acc[...] = jnp.zeros_like(acc)

    def tile(i, carry):
        at = pl.ds(pl.multiple_of(i * step, step), step)
        upper, lower = split(jnp.dot(x[at, :], factor[...], preferred_element_type=F32))
        g, s = gcot[at, :], scot[at, :]
        acc[:, :gc] += over_rows(upper[:, :rank], g) + over_rows(lower[:, :rank], g)
        acc[:, gc:] += over_rows(upper[:, rank:], s) + over_rows(lower[:, rank:], s)
        return carry

    lax.fori_loop(0, tiles, tile, 0)

    def part_of(block):
        return acc[pl.ds(pl.multiple_of(block * r, r), r), :]

    out_order = list(range(1, depth)) + [0]
    y_copies = {}
    for k in out_order:
        send_y[k] = part_of(2 * ((z + k) % depth) + 1 - y).astype(BF16)
        y_copies[k] = remote(send_y.at[k], recv_y.at[k], ry_send.at[k], ry_recv.at[k], (partner, t))
        y_copies[k].start()
    ring_step(1, (1,))

    grams = []
    for k in (0, 1):
        part = factor[:, k * rank:(k + 1) * rank]
        grams.append(split(over_rows(part, part)))

    z_copies = {}
    for k in range(1, depth):
        y_copies[k].wait_recv()
        send_z[k] = (part_of(along_z(k)) + recv_y[k].astype(F32)).astype(BF16)
        z_copies[k] = remote(send_z.at[k], recv_z.at[k], rz_send.at[k], rz_recv.at[k], (along_z(k), t))
        z_copies[k].start()

    ring_step(2, (0,))

    for c in loads[7:]:
        c.wait()
    y_copies[0].wait_recv()
    total = part_of(me) + recv_y[0].astype(F32)
    for k in range(1, depth):
        z_copies[k].wait_recv()
        total = total + recv_z[k].astype(F32)
    new_first = 0.8 * first[...] + 0.2 * total
    new_second = 0.9 * second[...] + 0.1 * total * total
    fnew[...] = new_first
    snew[...] = new_second
    dirs[me] = (new_first / jnp.sqrt(new_second)).astype(BF16)
    view = lambda b: dirs.at[b]
    d_copies = first_leg(view, d_send, d_recv)
    for k in order:
        d_copies[k].wait_recv()
        pass_over(d_copies, view, d_send, d_recv, k)

    ring_step(2, (1,))
    for k in range(depth):
        d_copies[depth + k].wait_recv()
    both = dirs[...].reshape(n * r, dirs.shape[2])
    squares = []
    for (upper, lower), part in zip(grams, (both[:, :gc], both[:, gc:])):
        lifted = jnp.dot(upper, part, preferred_element_type=F32)
        lifted = lifted + jnp.dot(lower, part, preferred_element_type=F32)
        squares.append(jnp.sum(part.astype(F32) * lifted))
    row = lax.broadcasted_iota(jnp.int32, sums.shape, 0)
    sums[...] = jnp.where(row == 0, squares[0], squares[1])
    s_copies = []
    for d in range(1, tp):
        c = remote(sums, sums_in.at[d], s_send.at[d], s_recv.at[d], (me, (t + d) % tp))
        c.start()
        s_copies.append(c)

    for s in range(3, steps):
        ring_step(s)
    for c in s_copies:
        c.wait()
    whole = sums[...]
    for d in range(1, tp):
        whole = whole + sums_in[d]
    gscale = 0.02 / jnp.sqrt(whole[0:1, 0:1] / sizes[0] + 0.25)
    sscale = 0.02 / jnp.sqrt(whole[1:2, 0:1] / sizes[1] + 0.25)
    gdir, sdir = both[:, :gc], both[:, gc:]

    def updates(block, at):
        f = f_all[block, at, :]
        return (
            gscale * jnp.dot(f[:, :rank], gdir, preferred_element_type=F32),
            sscale * jnp.dot(f[:, rank:], sdir, preferred_element_type=F32),
        )

    def refresh(block, at):
        gstep, sstep = updates(block, at)
        wout[block, at, :gc] = (wg[block, at, :gc].astype(F32) - gstep).astype(BF16)
        wout[block, at, gc:] = (wg[block, at, gc:].astype(F32) - sstep).astype(BF16)

    every = pl.ds(0, rows)
    gstep, sstep = updates(me, every)
    wnew[:, :gc] = wide[:, :gc] - gstep
    wnew[:, gc:] = wide[:, gc:] - sstep
    wout[me] = wnew[...].astype(BF16)
    for s in range(1, steps):
        refresh(at_pos(pos - s), every)
        refresh(at_pos(pos + s), every)
    for way in (0, 1):
        for h in halves(way, steps - 1):
            w_copies[way, steps - 1, h].wait_recv()
            refresh(at_pos(pos + steps), pl.ds(h * half, half))
    for group in (w_copies, f_copies, y_copies, z_copies, d_copies):
        for c in group.values():
            c.wait_send()
    for trio in shares.values():
        for c in trio:
            c.wait_send()


def finish_kernel(wout, wnew, fnew, snew, gnew, snew_w, gcopy, scopy, gf_out, gs_out, sf_out, ss_out, sems):
    gc = gnew.shape[1]
    sc = snew_w.shape[1]
    n, rows, _ = wout.shape
    left, right = pl.ds(0, gc), pl.ds(gc, sc)
    pairs = []
    for b in range(n):
        at = pl.ds(b * rows, rows)
        pairs.append((wout.at[b, :, left], gcopy.at[at, :]))
        pairs.append((wout.at[b, :, right], scopy.at[at, :]))
    for src, gate, state in ((wnew, gnew, snew_w), (fnew, gf_out, sf_out), (snew, gs_out, ss_out)):
        pairs.append((src.at[:, left], gate))
        pairs.append((src.at[:, right], state))
    copies = [pltpu.make_async_copy(src, dst, sems.at[k]) for k, (src, dst) in enumerate(pairs)]
    for c in copies:
        c.start()
    for c in copies:
        c.wait()


def per_device(
    n, tp, inputs, gate_cot, state_cot, gate_weight, state_weight, gate_factor, state_factor,
    gate_first, gate_second, state_first, state_second,
):
    args = (
        inputs, gate_cot, state_cot, gate_weight, state_weight, gate_factor, state_factor,
        gate_first, gate_second, state_first, state_second,
    )
    tokens, d = inputs.shape
    rows, gc = gate_weight.shape
    sc = state_weight.shape[1]
    cols = gc + sc
    rank = gate_factor.shape[1]
    r = gate_first.shape[0]
    tiles = 3 if tokens % (3 * 128) == 0 else 1
    dma = pltpu.SemaphoreType.DMA
    anys = pl.BlockSpec(memory_space=pltpu.HBM)
    sds = jax.ShapeDtypeStruct
    steps = n // 2
    sizes = (n * rows * gc * tp, n * rows * sc * tp)
    held = pl.pallas_call(
        functools.partial(exchange_kernel, n, tp, tiles, sizes),
        out_shape=(
            pltpu.VMEM((n, rows, cols), BF16),
            pltpu.VMEM((rows, cols), F32),
            pltpu.VMEM((r, cols), F32),
            pltpu.VMEM((r, cols), F32),
        ),
        in_specs=[anys] * 11,
        out_specs=[pl.BlockSpec(memory_space=pltpu.VMEM)] * 4,
        scratch_shapes=[
            pltpu.VMEM((n, rows, cols), BF16),
            pltpu.VMEM((n, rows, 2 * rank), BF16),
            pltpu.VMEM((n, r, cols), BF16),
            pltpu.VMEM((tokens, d), BF16),
            pltpu.VMEM((tokens, gc), BF16),
            pltpu.VMEM((tokens, sc), BF16),
            pltpu.VMEM((rows, cols), F32),
            pltpu.VMEM((rows, cols), BF16),
            pltpu.VMEM((r, cols), F32),
            pltpu.VMEM((r, cols), F32),
            pltpu.VMEM((rank, cols), F32),
        ]
        + [pltpu.VMEM((steps, r, cols), BF16)] * 4
        + [
            pltpu.VMEM((8, 128), F32),
            pltpu.VMEM((tp, 8, 128), F32),
            dma((11,)),
        ]
        + [dma((n,))] * 8
        + [dma((steps,))] * 4
        + [dma((n,))] * 2
        + [dma((tp,))] * 2
        + [dma((2, steps, 2))] * 2,
        compiler_params=pltpu.CompilerParams(
            collective_id=0, has_side_effects=True, vmem_limit_bytes=40 * 1024 * 1024
        ),
        name="exchange",
    )(*(pltpu.with_memory_space_constraint(a, pltpu.HBM) for a in args))

    outs = (gate_weight, state_weight, None, None, gate_first, gate_second, state_first, state_second)
    copies = (sds((n * rows, gc), BF16), sds((n * rows, sc), BF16))
    shapes = [sds(a.shape, a.dtype) for a in outs[:2]] + list(copies) + [sds(a.shape, a.dtype) for a in outs[4:]]
    return tuple(pl.pallas_call(
        finish_kernel,
        out_shape=tuple(shapes),
        in_specs=[pl.BlockSpec(memory_space=pltpu.VMEM)] * 4,
        out_specs=[anys] * 8,
        scratch_shapes=[dma((2 * n + 6,))],
        compiler_params=pltpu.CompilerParams(vmem_limit_bytes=4 * 1024 * 1024),
        name="finish",
    )(*(pltpu.with_memory_space_constraint(a, pltpu.VMEM) for a in held)))


def lifted_product(inputs, factor, cot):
    upper, lower = split(jnp.dot(inputs, factor, preferred_element_type=F32))
    first_part = jnp.einsum("tr,tc->rc", upper, cot, preferred_element_type=F32)
    return first_part + jnp.einsum("tr,tc->rc", lower, cot, preferred_element_type=F32)


def with_collectives(
    n, tp, inputs, gate_cot, state_cot, gate_weight, state_weight, gate_factor, state_factor,
    gate_first, gate_second, state_first, state_second,
):
    gc = gate_cot.shape[1]
    gate_part = lifted_product(inputs, lax.all_gather(gate_factor, "fs", axis=0, tiled=True), gate_cot)
    state_part = lifted_product(inputs, lax.all_gather(state_factor, "fs", axis=0, tiled=True), state_cot)
    partial_proj = jnp.concatenate([gate_part, state_part], 1)
    projection = lax.psum_scatter(partial_proj, "fs", scatter_dimension=0, tiled=True)
    first_new = 0.8 * jnp.concatenate([gate_first, state_first], 1) + 0.2 * projection
    second_new = 0.9 * jnp.concatenate([gate_second, state_second], 1) + 0.1 * projection * projection
    direction = (first_new / jnp.sqrt(second_new)).astype(BF16)
    dirs = lax.all_gather(direction, "fs", axis=0, tiled=True)
    gate_full = jnp.dot(gate_factor, dirs[:, :gc], preferred_element_type=F32)
    state_full = jnp.dot(state_factor, dirs[:, gc:], preferred_element_type=F32)
    gate_sq, state_sq = lax.psum(
        (jnp.sum(gate_full * gate_full), jnp.sum(state_full * state_full)), ("fs", "tp")
    )
    gate_scale = 0.02 / jnp.sqrt(gate_sq / (gate_full.size * n * tp) + 0.25)
    state_scale = 0.02 / jnp.sqrt(state_sq / (state_full.size * n * tp) + 0.25)
    gate_new = gate_weight - gate_scale * gate_full
    state_new = state_weight - state_scale * state_full
    gate_copy = lax.all_gather(gate_new.astype(BF16), "fs", axis=0, tiled=True)
    state_copy = lax.all_gather(state_new.astype(BF16), "fs", axis=0, tiled=True)
    return (
        gate_new, state_new, gate_copy, state_copy,
        first_new[:, :gc], second_new[:, :gc], first_new[:, gc:], second_new[:, gc:],
    )


def solution(mesh):
    n, tp = mesh.shape["fs"], mesh.shape["tp"]
    both = P("fs", "tp")
    wide = P("fs", None)

    def body(*args):
        r = args[7].shape[0]
        quarter = args[5].shape[0] // tp
        fits = tp == 4 and r % 16 == 0 and quarter % 16 == 0 and n >= 8
        return (per_device if fits else with_collectives)(n, tp, *args)

    return jax.shard_map(
        body,
        mesh=mesh,
        in_specs=(wide, both, both, both, both, wide, wide, both, both, both, both),
        out_specs=(both, both, P(None, "tp"), P(None, "tp"), both, both, both, both),
        check_vma=False,
    )
```

```python
import functools

import jax
import jax.numpy as jnp
from jax import lax
from jax.experimental import pallas as pl
from jax.experimental.pallas import tpu as pltpu
from jax.sharding import PartitionSpec as P

MESH = pl.DeviceIdType.MESH
BF16 = jnp.bfloat16
F32 = jnp.float32

PLACE = {'a': (0, 1), 'b2': (2,), 'd1': (3, 4), 'd6': (5,), 'e': (6,), 'r1': (7,), 'q0': (8,), 't': (9,), 'u1': (10,), 'u2': (11,), 'u3': (12,), 'v1': (13,), 'w': (14, 15)}


def over_rows(a, b):
    return lax.dot_general(a, b, (((0,), (0,)), ((), ())), preferred_element_type=F32)


def split(a):
    upper = a.astype(BF16)
    return upper, (a - upper.astype(F32)).astype(BF16)


def exchange_kernel(
    n, tp, tiles, sizes,
    x_hbm, gcot_hbm, scot_hbm, gw_hbm, sw_hbm, gf_hbm, sf_hbm, gfirst_hbm, gsecond_hbm, sfirst_hbm, ssecond_hbm,
    wout, wnew, fnew, snew,
    wg, f_all, dirs, x, gcot, scot, wide, wown, first, second, total, acc, send_y, recv_y, send_z, recv_z, sums, sums_in,
    load,
    f_send, f_recv, fx_send, fx_recv, fc_send, fc_recv, fd_send, fd_recv,
    ry_send, ry_recv, rz_send, rz_recv, d_send, d_recv, dy_send, dy_recv, s_send, s_recv, w_send, w_recv,
):
    me = lax.axis_index("fs")
    t = lax.axis_index("tp")
    rows, rank = gf_hbm.shape
    gc = gcot.shape[1]
    sc = scot.shape[1]
    r = first.shape[0]
    q = rows // tp
    depth = n // 2
    z, y = me // 2, me % 2
    partner = 2 * z + 1 - y

    sources = [
        (gf_hbm, f_all.at[me, :, pl.ds(0, rank)]),
        (sf_hbm, f_all.at[me, :, pl.ds(rank, rank)]),
        (gw_hbm, wide.at[:, pl.ds(0, gc)]),
        (sw_hbm, wide.at[:, pl.ds(gc, sc)]),
        (x_hbm, x),
        (gcot_hbm, gcot),
        (scot_hbm, scot),
        (gfirst_hbm, first.at[:, pl.ds(0, gc)]),
        (sfirst_hbm, first.at[:, pl.ds(gc, sc)]),
        (gsecond_hbm, second.at[:, pl.ds(0, gc)]),
        (ssecond_hbm, second.at[:, pl.ds(gc, sc)]),
    ]
    loads = [pltpu.make_async_copy(src, dst, load.at[k]) for k, (src, dst) in enumerate(sources)]
    for c in loads:
        c.start()

    def along_z(k):
        return 2 * ((z + depth + k) % depth) + y

    barrier = pltpu.get_barrier_semaphore()
    pl.semaphore_signal(barrier, inc=1, device_id=(partner, t), device_id_type=MESH)
    for k in range(1, depth):
        pl.semaphore_signal(barrier, inc=1, device_id=(along_z(k), t), device_id_type=MESH)
    for d in range(1, tp):
        pl.semaphore_signal(barrier, inc=1, device_id=(me, (t + d) % tp), device_id_type=MESH)
    pl.semaphore_wait(barrier, depth + tp - 1)

    def remote(src, dst, ss, rs, dev):
        return pltpu.make_async_remote_copy(
            src_ref=src, dst_ref=dst, send_sem=ss, recv_sem=rs, device_id=dev, device_id_type=MESH
        )

    core_peer = t + 1 - 2 * (t % 2)
    x_peer = (t + 2) % tp

    def source_block(j):
        k = j % depth
        return 2 * ((z + depth - k) % depth) + (y if j < depth else 1 - y)

    def quarter(block, which):
        return f_all.at[block, pl.ds(which * q, q), :]

    def first_leg(view, send, recv):
        copies = {}
        for j in sorted(range(1, depth), key=lambda k: -min(k, depth - k)) + [depth]:
            dev = partner if j == depth else along_z(j)
            copies[j] = remote(view(me), view(me), send.at[j], recv.at[j], (dev, t))
            copies[j].start()
        return copies

    def pass_over(copies, view, send, recv, k):
        b = source_block(k)
        copies[depth + k] = remote(
            view(b), view(b), send.at[depth + k], recv.at[depth + k], (partner, t)
        )
        copies[depth + k].start()

    loads[0].wait()
    loads[1].wait()
    mine = lambda b: quarter(b, t)
    f_copies = first_leg(mine, f_send, f_recv)

    loads[2].wait()
    loads[3].wait()
    wown[...] = wide[...].astype(BF16)

    pos = z + y * (n - 1 - 2 * z)

    def at_pos(p):
        p = (p + n) % n
        far = p // (n // 2)
        return 2 * p * (1 - far) + far * (2 * (n - 1 - p) + 1)

    right, left = at_pos(pos + 1), at_pos(pos - 1)
    steps = n // 2

    parts = 4
    piece = rows // parts

    def w_copy(way, s, h):
        block = at_pos(pos - s) if way == 0 else at_pos(pos + s)
        at = pl.ds(h * piece, piece)
        dst = wg.at[block, at, :]
        src = wown.at[at, :] if s == 0 else dst
        return remote(
            src, dst, w_send.at[way, s, h], w_recv.at[way, s, h], (right if way == 0 else left, t)
        )

    def last_pieces(way):
        return range(parts // 2) if way == 0 else range(parts // 2, parts)

    w_copies = {}

    def tick(i):
        s, k = i // parts, i % parts
        for way in (0, 1):
            h = k if way == 0 else parts - 1 - k
            if s > 0:
                w_copies[way, s - 1, h].wait_recv()
            if s < steps - 1 or h in last_pieces(way):
                w_copies[way, s, h] = w_copy(way, s, h)
                w_copies[way, s, h].start()

    def ticks(name):
        for i in PLACE.get(name, ()):
            tick(i)

    ticks('a')

    shares = {}

    def share(j):
        src = quarter(source_block(j), t)
        cx = remote(src, src, fx_send.at[j], fx_recv.at[j], (me, x_peer))
        cx.start()
        cc = remote(src, src, fc_send.at[j], fc_recv.at[j], (me, core_peer))
        cc.start()
        shares[j] = [cx, cc]

    order = sorted(range(1, depth), key=lambda k: min(k, depth - k))
    for k in order:
        f_copies[k].wait_recv()
        pass_over(f_copies, mine, f_send, f_recv, k)
        share(k)
        if k == order[0]:
            f_copies[depth].wait_recv()
            share(depth)
        ticks(f'b{k}')

    for k in order:
        f_copies[depth + k].wait_recv()
        share(depth + k)
        ticks(f'c{k}')
    for j, pair in shares.items():
        pair[0].wait_recv()
        src = quarter(source_block(j), x_peer)
        cd = remote(src, src, fd_send.at[j], fd_recv.at[j], (me, core_peer))
        cd.start()
        pair.append(cd)
        ticks(f'd{j}')
    for cx, cc, cd in shares.values():
        cc.wait_recv()
        cd.wait_recv()

    ticks('d')
    for k in (4, 5, 6):
        loads[k].wait()
    factor = f_all.reshape(n * rows, 2 * rank)
    step = x.shape[0] // tiles
    acc[...] = jnp.zeros_like(acc)

    for i in range(tiles):
        at = pl.ds(i * step, step)
        upper, lower = split(jnp.dot(x[at, :], factor[...], preferred_element_type=F32))
        g, s = gcot[at, :], scot[at, :]
        acc[:, :gc] += over_rows(upper[:, :rank], g) + over_rows(lower[:, :rank], g)
        acc[:, gc:] += over_rows(upper[:, rank:], s) + over_rows(lower[:, rank:], s)
        ticks(f'm{i}')

    def part_of(block):
        return acc[pl.ds(pl.multiple_of(block * r, r), r), :]

    low = z < depth // 2
    flip = 1 - low.astype(jnp.int32)
    zz = z + flip * (depth - 1 - 2 * z)
    ahead = z + 1 - 2 * flip
    behind = z - 1 + 2 * flip

    def level(k):
        return k + flip * (depth - 1 - 2 * k)

    y_copies = {}
    for k in reversed(range(depth)):
        send_y[k] = part_of(2 * level(k) + 1 - y).astype(BF16)
        y_copies[k] = remote(send_y.at[k], recv_y.at[k], ry_send.at[k], ry_recv.at[k], (partner, t))
        y_copies[k].start()
    ticks('e')

    grams = []
    for k in (0, 1):
        part = factor[:, k * rank:(k + 1) * rank]
        grams.append(split(over_rows(part, part)))

    ticks('g')
    def hop(way, k, target):
        goal = level(k)
        return remote(
            send_z.at[goal], recv_z.at[way, goal], rz_send.at[goal], rz_recv.at[way, goal],
            (2 * target + y, t),
        )

    def add_on(total, way, k):
        hop(way, k, z).wait_recv()
        return total + recv_z[way, level(k)].astype(F32)

    def both_rows(k):
        y_copies[k].wait_recv()
        return part_of(2 * level(k) + y) + recv_y[k].astype(F32)

    def pass_up(k):
        @pl.when(zz > 0)
        def _():
            send_z[level(k)] = add_on(both_rows(k), flip, k).astype(BF16)

        @pl.when(zz == 0)
        def _():
            send_z[level(k)] = both_rows(k).astype(BF16)

        hop(flip, k, ahead).start()

    for k in reversed(range(1, depth)):
        pl.when(zz < k)(functools.partial(pass_up, k))
        ticks(f'r{k}')
    for k in range(depth // 2 - 1):
        @pl.when(zz > k)
        def _():
            send_z[level(k)] = add_on(both_rows(k), 1 - flip, k).astype(BF16)
            hop(1 - flip, k, behind).start()
        ticks(f'q{k}')

    ticks('s')

    for c in loads[7:]:
        c.wait()
    for k in range(depth // 2):
        @pl.when(zz == k)
        def _():
            total[...] = add_on(both_rows(k), 1 - flip, k)
            if k > 0:
                total[...] = add_on(total[...], flip, k)

    proj = total[...]
    new_first = 0.8 * first[...] + 0.2 * proj
    new_second = 0.9 * second[...] + 0.1 * proj * proj
    fnew[...] = new_first
    snew[...] = new_second
    dirs[me] = (new_first / jnp.sqrt(new_second)).astype(BF16)
    def d_hop(way, j):
        origin = z + 1 - j if way == 0 else z - 1 + j
        view = dirs.at[2 * origin + y]
        target = z + 1 if way == 0 else z - 1
        return remote(view, view, d_send.at[way, j], d_recv.at[way, j], (2 * target + y, t))

    def d_in(way, j):
        origin = z - j if way == 0 else z + j
        view = dirs.at[2 * origin + y]
        return remote(view, view, d_send.at[way, j], d_recv.at[way, j], (me, t))

    def d_over(way, j):
        origin = z - j if way == 0 else z + j
        view = dirs.at[2 * origin + y]
        return remote(view, view, dy_send.at[way, j], dy_recv.at[way, j], (partner, t))

    def d_over_in(way, j):
        origin = z - j if way == 0 else z + j
        view = dirs.at[2 * origin + 1 - y]
        return remote(view, view, dy_send.at[way, j], dy_recv.at[way, j], (partner, t))

    def there(way, j):
        return z >= j if way == 0 else z < depth - j

    def more(way):
        return there(1 - way, 1)

    for way in (0, 1):
        pl.when(more(way))(d_hop(way, 1).start)
    d_over(0, 0).start()
    ticks('t')
    for j in range(1, depth):
        for way in (0, 1):
            @pl.when(there(way, j))
            def _():
                d_in(way, j).wait_recv()
                if j < depth - 1:
                    pl.when(more(way))(d_hop(way, j + 1).start)
                d_over(way, j).start()
        ticks(f'u{j}')

    ticks('v')
    d_over_in(0, 0).wait_recv()
    for j in range(1, depth):
        for way in (0, 1):
            pl.when(there(way, j))(d_over_in(way, j).wait_recv)
        ticks(f'v{j}')
    both = dirs[...].reshape(n * r, dirs.shape[2])
    squares = []
    for (upper, lower), part in zip(grams, (both[:, :gc], both[:, gc:])):
        lifted = jnp.dot(upper, part, preferred_element_type=F32)
        lifted = lifted + jnp.dot(lower, part, preferred_element_type=F32)
        squares.append(jnp.sum(part.astype(F32) * lifted))
    row = lax.broadcasted_iota(jnp.int32, sums.shape, 0)
    sums[...] = jnp.where(row == 0, squares[0], squares[1])
    s_copies = []
    for d in range(1, tp):
        c = remote(sums, sums_in.at[d], s_send.at[d], s_recv.at[d], (me, (t + d) % tp))
        c.start()
        s_copies.append(c)

    ticks('w')
    for c in s_copies:
        c.wait()
    whole = sums[...]
    for d in range(1, tp):
        whole = whole + sums_in[d]
    gscale = 0.02 / jnp.sqrt(whole[0:1, 0:1] / sizes[0] + 0.25)
    sscale = 0.02 / jnp.sqrt(whole[1:2, 0:1] / sizes[1] + 0.25)
    gdir, sdir = both[:, :gc], both[:, gc:]

    def updates(block, at):
        f = f_all[block, at, :]
        return (
            gscale * jnp.dot(f[:, :rank], gdir, preferred_element_type=F32),
            sscale * jnp.dot(f[:, rank:], sdir, preferred_element_type=F32),
        )

    def refresh(block, at):
        gstep, sstep = updates(block, at)
        wout[block, at, :gc] = (wg[block, at, :gc].astype(F32) - gstep).astype(BF16)
        wout[block, at, gc:] = (wg[block, at, gc:].astype(F32) - sstep).astype(BF16)

    every = pl.ds(0, rows)
    gstep, sstep = updates(me, every)
    wnew[:, :gc] = wide[:, :gc] - gstep
    wnew[:, gc:] = wide[:, gc:] - sstep
    wout[me] = wnew[...].astype(BF16)
    for s in range(1, steps):
        refresh(at_pos(pos - s), every)
        refresh(at_pos(pos + s), every)
    ticks('x')
    for way in (0, 1):
        for h in last_pieces(way):
            w_copies[way, steps - 1, h].wait_recv()
        at = pl.ds(way * (rows // 2), rows // 2)
        refresh(at_pos(pos + steps), at)
    for c in w_copies.values():
        c.wait_send()
    for group in (f_copies, y_copies):
        for c in group.values():
            c.wait_send()
    for k in range(1, depth):
        pl.when(zz < k)(hop(flip, k, ahead).wait_send)
    for k in range(depth // 2 - 1):
        pl.when(zz > k)(hop(1 - flip, k, behind).wait_send)
    d_over(0, 0).wait_send()
    for way in (0, 1):
        for j in range(1, depth):
            pl.when(more(way) & there(way, j - 1))(d_hop(way, j).wait_send)
            pl.when(there(way, j))(d_over(way, j).wait_send)
    for trio in shares.values():
        for c in trio:
            c.wait_send()


def finish_kernel(wout, wnew, fnew, snew, gnew, snew_w, gcopy, scopy, gf_out, gs_out, sf_out, ss_out, sems):
    gc = gnew.shape[1]
    sc = snew_w.shape[1]
    n, rows, _ = wout.shape
    left, right = pl.ds(0, gc), pl.ds(gc, sc)
    pairs = []
    for b in range(n):
        at = pl.ds(b * rows, rows)
        pairs.append((wout.at[b, :, left], gcopy.at[at, :]))
        pairs.append((wout.at[b, :, right], scopy.at[at, :]))
    for src, gate, state in ((wnew, gnew, snew_w), (fnew, gf_out, sf_out), (snew, gs_out, ss_out)):
        pairs.append((src.at[:, left], gate))
        pairs.append((src.at[:, right], state))
    copies = [pltpu.make_async_copy(src, dst, sems.at[k]) for k, (src, dst) in enumerate(pairs)]
    for c in copies:
        c.start()
    for c in copies:
        c.wait()


def per_device(
    n, tp, inputs, gate_cot, state_cot, gate_weight, state_weight, gate_factor, state_factor,
    gate_first, gate_second, state_first, state_second,
):
    args = (
        inputs, gate_cot, state_cot, gate_weight, state_weight, gate_factor, state_factor,
        gate_first, gate_second, state_first, state_second,
    )
    tokens, d = inputs.shape
    rows, gc = gate_weight.shape
    sc = state_weight.shape[1]
    cols = gc + sc
    rank = gate_factor.shape[1]
    r = gate_first.shape[0]
    tiles = 3 if tokens % (3 * 128) == 0 else 1
    dma = pltpu.SemaphoreType.DMA
    anys = pl.BlockSpec(memory_space=pltpu.HBM)
    sds = jax.ShapeDtypeStruct
    steps = n // 2
    sizes = (n * rows * gc * tp, n * rows * sc * tp)
    held = pl.pallas_call(
        functools.partial(exchange_kernel, n, tp, tiles, sizes),
        out_shape=(
            pltpu.VMEM((n, rows, cols), BF16),
            pltpu.VMEM((rows, cols), F32),
            pltpu.VMEM((r, cols), F32),
            pltpu.VMEM((r, cols), F32),
        ),
        in_specs=[anys] * 11,
        out_specs=[pl.BlockSpec(memory_space=pltpu.VMEM)] * 4,
        scratch_shapes=[
            pltpu.VMEM((n, rows, cols), BF16),
            pltpu.VMEM((n, rows, 2 * rank), BF16),
            pltpu.VMEM((n, r, cols), BF16),
            pltpu.VMEM((tokens, d), BF16),
            pltpu.VMEM((tokens, gc), BF16),
            pltpu.VMEM((tokens, sc), BF16),
            pltpu.VMEM((rows, cols), F32),
            pltpu.VMEM((rows, cols), BF16),
            pltpu.VMEM((r, cols), F32),
            pltpu.VMEM((r, cols), F32),
            pltpu.VMEM((r, cols), F32),
            pltpu.VMEM((rank, cols), F32),
        ]
        + [pltpu.VMEM((steps, r, cols), BF16)] * 3
        + [pltpu.VMEM((2, steps, r, cols), BF16)]
        + [
            pltpu.VMEM((8, 128), F32),
            pltpu.VMEM((tp, 8, 128), F32),
            dma((11,)),
        ]
        + [dma((n,))] * 8
        + [dma((steps,))] * 3
        + [dma((2, steps))] * 5
        + [dma((tp,))] * 2
        + [dma((2, steps, 4))] * 2,
        compiler_params=pltpu.CompilerParams(
            collective_id=0, has_side_effects=True, vmem_limit_bytes=40 * 1024 * 1024
        ),
        name="exchange",
    )(*(pltpu.with_memory_space_constraint(a, pltpu.HBM) for a in args))

    outs = (gate_weight, state_weight, None, None, gate_first, gate_second, state_first, state_second)
    copies = (sds((n * rows, gc), BF16), sds((n * rows, sc), BF16))
    shapes = [sds(a.shape, a.dtype) for a in outs[:2]] + list(copies) + [sds(a.shape, a.dtype) for a in outs[4:]]
    return tuple(pl.pallas_call(
        finish_kernel,
        out_shape=tuple(shapes),
        in_specs=[pl.BlockSpec(memory_space=pltpu.VMEM)] * 4,
        out_specs=[anys] * 8,
        scratch_shapes=[dma((2 * n + 6,))],
        compiler_params=pltpu.CompilerParams(vmem_limit_bytes=4 * 1024 * 1024),
        name="finish",
    )(*(pltpu.with_memory_space_constraint(a, pltpu.VMEM) for a in held)))


def lifted_product(inputs, factor, cot):
    upper, lower = split(jnp.dot(inputs, factor, preferred_element_type=F32))
    first_part = jnp.einsum("tr,tc->rc", upper, cot, preferred_element_type=F32)
    return first_part + jnp.einsum("tr,tc->rc", lower, cot, preferred_element_type=F32)


def with_collectives(
    n, tp, inputs, gate_cot, state_cot, gate_weight, state_weight, gate_factor, state_factor,
    gate_first, gate_second, state_first, state_second,
):
    gc = gate_cot.shape[1]
    gate_part = lifted_product(inputs, lax.all_gather(gate_factor, "fs", axis=0, tiled=True), gate_cot)
    state_part = lifted_product(inputs, lax.all_gather(state_factor, "fs", axis=0, tiled=True), state_cot)
    partial_proj = jnp.concatenate([gate_part, state_part], 1)
    projection = lax.psum_scatter(partial_proj, "fs", scatter_dimension=0, tiled=True)
    first_new = 0.8 * jnp.concatenate([gate_first, state_first], 1) + 0.2 * projection
    second_new = 0.9 * jnp.concatenate([gate_second, state_second], 1) + 0.1 * projection * projection
    direction = (first_new / jnp.sqrt(second_new)).astype(BF16)
    dirs = lax.all_gather(direction, "fs", axis=0, tiled=True)
    gate_full = jnp.dot(gate_factor, dirs[:, :gc], preferred_element_type=F32)
    state_full = jnp.dot(state_factor, dirs[:, gc:], preferred_element_type=F32)
    gate_sq, state_sq = lax.psum(
        (jnp.sum(gate_full * gate_full), jnp.sum(state_full * state_full)), ("fs", "tp")
    )
    gate_scale = 0.02 / jnp.sqrt(gate_sq / (gate_full.size * n * tp) + 0.25)
    state_scale = 0.02 / jnp.sqrt(state_sq / (state_full.size * n * tp) + 0.25)
    gate_new = gate_weight - gate_scale * gate_full
    state_new = state_weight - state_scale * state_full
    gate_copy = lax.all_gather(gate_new.astype(BF16), "fs", axis=0, tiled=True)
    state_copy = lax.all_gather(state_new.astype(BF16), "fs", axis=0, tiled=True)
    return (
        gate_new, state_new, gate_copy, state_copy,
        first_new[:, :gc], second_new[:, :gc], first_new[:, gc:], second_new[:, gc:],
    )


def solution(mesh):
    n, tp = mesh.shape["fs"], mesh.shape["tp"]
    both = P("fs", "tp")
    wide = P("fs", None)

    def body(*args):
        r = args[7].shape[0]
        quarter = args[5].shape[0] // tp
        fits = tp == 4 and r % 16 == 0 and quarter % 16 == 0 and n >= 8
        return (per_device if fits else with_collectives)(n, tp, *args)

    return jax.shard_map(
        body,
        mesh=mesh,
        in_specs=(wide, both, both, both, both, wide, wide, both, both, both, both),
        out_specs=(both, both, P(None, "tp"), P(None, "tp"), both, both, both, both),
        check_vma=False,
    )
```

```python
import functools

import jax
import jax.numpy as jnp
from jax import lax
from jax.experimental import pallas as pl
from jax.experimental.pallas import tpu as pltpu
from jax.sharding import PartitionSpec as P

MESH = pl.DeviceIdType.MESH
BF16 = jnp.bfloat16
F32 = jnp.float32

KINDS = "omiy"
PLACE = {'a': ((0, 'omiy'), (1, 'miy'), (2, 'mi'), (3, 'mi')), 'c1': ((2, 'y'), (3, 'y'), (4, 'y'), (5, 'm')), 'd1': ((5, 'y'), (6, 'm')), 'r2': ((6, 'y'), (7, 'y'), (8, 'y'), (9, 'y')), 'r1': ((8, 'm'), (10, 'y')), 'v': ((11, 'y'),), 'v2': ((12, 'y'), (13, 'o'), (14, 'i')), 'w': ((13, 'my'), (14, 'omy'), (15, 'omy')), 'b3': ((1, 'o'), (2, 'o'), (3, 'o'), (4, 'm')), 'c2': ((4, 'o'), (5, 'o')), 'd3': ((6, 'o'),), 'q0': ((7, 'o'), (8, 'o')), 't': ((9, 'om'), (10, 'o'), (11, 'o'), (12, 'o')), 'b2': ((4, 'i'),), 'd5': ((5, 'i'),), 'd': ((6, 'i'),), 'g': ((7, 'i'), (8, 'i'), (9, 'i')), 's': ((10, 'i'),), 'u1': ((10, 'm'), (11, 'i')), 'u3': ((11, 'm'), (12, 'i'), (13, 'i')), 'v3': ((15, 'i'),), 'm0': ((7, 'm'),), 'v1': ((12, 'm'),)}


def over_rows(a, b):
    return lax.dot_general(a, b, (((0,), (0,)), ((), ())), preferred_element_type=F32)


def split(a):
    upper = a.astype(BF16)
    return upper, (a - upper.astype(F32)).astype(BF16)


def exchange_kernel(
    n, tp, tiles, sizes,
    x_hbm, gcot_hbm, scot_hbm, gw_hbm, sw_hbm, gf_hbm, sf_hbm, gfirst_hbm, gsecond_hbm, sfirst_hbm, ssecond_hbm,
    wout, wnew, fnew, snew,
    wg, f_all, dirs, x, gcot, scot, wide, wown, first, second, total, acc, send_y, recv_y, send_z, recv_z, sums, sums_in,
    load,
    f_send, f_recv, fx_send, fx_recv, fc_send, fc_recv, fd_send, fd_recv,
    ry_send, ry_recv, rz_send, rz_recv, d_send, d_recv, dy_send, dy_recv, s_send, s_recv, w_send, w_recv,
):
    me = lax.axis_index("fs")
    t = lax.axis_index("tp")
    rows, rank = gf_hbm.shape
    gc = gcot.shape[1]
    sc = scot.shape[1]
    r = first.shape[0]
    q = rows // tp
    depth = n // 2
    z, y = me // 2, me % 2
    partner = 2 * z + 1 - y

    sources = [
        (gf_hbm, f_all.at[me, :, pl.ds(0, rank)]),
        (sf_hbm, f_all.at[me, :, pl.ds(rank, rank)]),
        (gw_hbm, wide.at[:, pl.ds(0, gc)]),
        (sw_hbm, wide.at[:, pl.ds(gc, sc)]),
        (x_hbm, x),
        (gcot_hbm, gcot),
        (scot_hbm, scot),
        (gfirst_hbm, first.at[:, pl.ds(0, gc)]),
        (sfirst_hbm, first.at[:, pl.ds(gc, sc)]),
        (gsecond_hbm, second.at[:, pl.ds(0, gc)]),
        (ssecond_hbm, second.at[:, pl.ds(gc, sc)]),
    ]
    loads = [pltpu.make_async_copy(src, dst, load.at[k]) for k, (src, dst) in enumerate(sources)]
    for c in loads:
        c.start()

    def along_z(k):
        return 2 * ((z + depth + k) % depth) + y

    barrier = pltpu.get_barrier_semaphore()
    pl.semaphore_signal(barrier, inc=1, device_id=(partner, t), device_id_type=MESH)
    for k in range(1, depth):
        pl.semaphore_signal(barrier, inc=1, device_id=(along_z(k), t), device_id_type=MESH)
    for d in range(1, tp):
        pl.semaphore_signal(barrier, inc=1, device_id=(me, (t + d) % tp), device_id_type=MESH)
    pl.semaphore_wait(barrier, depth + tp - 1)

    def remote(src, dst, ss, rs, dev):
        return pltpu.make_async_remote_copy(
            src_ref=src, dst_ref=dst, send_sem=ss, recv_sem=rs, device_id=dev, device_id_type=MESH
        )

    core_peer = t + 1 - 2 * (t % 2)
    x_peer = (t + 2) % tp

    def source_block(j):
        k = j % depth
        return 2 * ((z + depth - k) % depth) + (y if j < depth else 1 - y)

    def quarter(block, which):
        return f_all.at[block, pl.ds(which * q, q), :]

    def first_leg(view, send, recv):
        copies = {}
        for j in sorted(range(1, depth), key=lambda k: -min(k, depth - k)) + [depth]:
            dev = partner if j == depth else along_z(j)
            copies[j] = remote(view(me), view(me), send.at[j], recv.at[j], (dev, t))
            copies[j].start()
        return copies

    def pass_over(copies, view, send, recv, k):
        b = source_block(k)
        copies[depth + k] = remote(
            view(b), view(b), send.at[depth + k], recv.at[depth + k], (partner, t)
        )
        copies[depth + k].start()

    loads[0].wait()
    loads[1].wait()
    mine = lambda b: quarter(b, t)
    f_copies = first_leg(mine, f_send, f_recv)

    loads[2].wait()
    loads[3].wait()
    wown[...] = wide[...].astype(BF16)

    pos = z + y * (n - 1 - 2 * z)

    def at_pos(p):
        p = (p + n) % n
        far = p // (n // 2)
        return 2 * p * (1 - far) + far * (2 * (n - 1 - p) + 1)

    right, left = at_pos(pos + 1), at_pos(pos - 1)
    steps = n // 2

    parts = 4
    piece = rows // parts

    def w_copy(way, s, h):
        block = at_pos(pos - s) if way == 0 else at_pos(pos + s)
        at = pl.ds(h * piece, piece)
        dst = wg.at[block, at, :]
        src = wown.at[at, :] if s == 0 else dst
        return remote(
            src, dst, w_send.at[way, s, h], w_recv.at[way, s, h], (right if way == 0 else left, t)
        )

    def in_first(p, h):
        p = (p + n) % n % steps
        share = parts // 2 - (p == 0).astype(jnp.int32) + (p == steps - 1).astype(jnp.int32)
        return h < share

    def sent(way, s, h):
        if s < steps - 1:
            return pos >= 0
        return in_first(pos + 1, h) if way == 0 else ~in_first(pos - 1, h)

    w_copies = {}

    spot = pos % steps

    def forward(way, s, k):
        h = k if way == 0 else parts - 1 - k
        if s > 0:
            w_copies[way, s - 1, h].wait_recv()
        if s < steps - 1:
            w_copies[way, s, h].start()
        elif k < parts - 1:
            pl.when(sent(way, s, h))(w_copies[way, s, h].start)

    def ticks(name):
        for i, kinds in PLACE.get(name, ()):
            s, k = i // parts, i % parts
            for way in (0, 1):
                h = k if way == 0 else parts - 1 - k
                if s < steps - 1 or k < parts - 1:
                    w_copies[way, s, h] = w_copy(way, s, h)
                if len(kinds) == len(KINDS):
                    forward(way, s, k)
                    continue
                for kind in kinds:
                    at = KINDS.index(kind)
                    at = at if way == 0 else steps - 1 - at
                    pl.when(spot == at)(functools.partial(forward, way, s, k))

    ticks('a')

    shares = {}

    def share(j):
        src = quarter(source_block(j), t)
        cx = remote(src, src, fx_send.at[j], fx_recv.at[j], (me, x_peer))
        cx.start()
        cc = remote(src, src, fc_send.at[j], fc_recv.at[j], (me, core_peer))
        cc.start()
        shares[j] = [cx, cc]

    order = sorted(range(1, depth), key=lambda k: min(k, depth - k))
    for k in order:
        f_copies[k].wait_recv()
        pass_over(f_copies, mine, f_send, f_recv, k)
        share(k)
        if k == order[0]:
            f_copies[depth].wait_recv()
            share(depth)
        ticks(f'b{k}')

    for k in order:
        f_copies[depth + k].wait_recv()
        share(depth + k)
        ticks(f'c{k}')
    for j, pair in shares.items():
        pair[0].wait_recv()
        src = quarter(source_block(j), x_peer)
        cd = remote(src, src, fd_send.at[j], fd_recv.at[j], (me, core_peer))
        cd.start()
        pair.append(cd)
        ticks(f'd{j}')
    for cx, cc, cd in shares.values():
        cc.wait_recv()
        cd.wait_recv()

    ticks('d')
    for k in (4, 5, 6):
        loads[k].wait()
    factor = f_all.reshape(n * rows, 2 * rank)
    step = x.shape[0] // tiles
    acc[...] = jnp.zeros_like(acc)

    for i in range(tiles):
        at = pl.ds(i * step, step)
        upper, lower = split(jnp.dot(x[at, :], factor[...], preferred_element_type=F32))
        g, s = gcot[at, :], scot[at, :]
        acc[:, :gc] += over_rows(upper[:, :rank], g) + over_rows(lower[:, :rank], g)
        acc[:, gc:] += over_rows(upper[:, rank:], s) + over_rows(lower[:, rank:], s)
        ticks(f'm{i}')

    def part_of(block):
        return acc[pl.ds(pl.multiple_of(block * r, r), r), :]

    low = z < depth // 2
    flip = 1 - low.astype(jnp.int32)
    zz = z + flip * (depth - 1 - 2 * z)
    ahead = z + 1 - 2 * flip
    behind = z - 1 + 2 * flip

    def level(k):
        return k + flip * (depth - 1 - 2 * k)

    y_copies = {}
    for k in reversed(range(depth)):
        send_y[k] = part_of(2 * level(k) + 1 - y).astype(BF16)
        y_copies[k] = remote(send_y.at[k], recv_y.at[k], ry_send.at[k], ry_recv.at[k], (partner, t))
        y_copies[k].start()
    ticks('e')

    grams = []
    for k in (0, 1):
        part = factor[:, k * rank:(k + 1) * rank]
        grams.append(split(over_rows(part, part)))

    ticks('g')
    def hop(way, k, target):
        goal = level(k)
        return remote(
            send_z.at[goal], recv_z.at[way, goal], rz_send.at[goal], rz_recv.at[way, goal],
            (2 * target + y, t),
        )

    def add_on(total, way, k):
        hop(way, k, z).wait_recv()
        return total + recv_z[way, level(k)].astype(F32)

    def both_rows(k):
        y_copies[k].wait_recv()
        return part_of(2 * level(k) + y) + recv_y[k].astype(F32)

    def pass_up(k):
        @pl.when(zz > 0)
        def _():
            send_z[level(k)] = add_on(both_rows(k), flip, k).astype(BF16)

        @pl.when(zz == 0)
        def _():
            send_z[level(k)] = both_rows(k).astype(BF16)

        hop(flip, k, ahead).start()

    for k in reversed(range(1, depth)):
        pl.when(zz < k)(functools.partial(pass_up, k))
        ticks(f'r{k}')
    for k in range(depth // 2 - 1):
        @pl.when(zz > k)
        def _():
            send_z[level(k)] = add_on(both_rows(k), 1 - flip, k).astype(BF16)
            hop(1 - flip, k, behind).start()
        ticks(f'q{k}')

    ticks('s')

    for c in loads[7:]:
        c.wait()
    for k in range(depth // 2):
        @pl.when(zz == k)
        def _():
            total[...] = add_on(both_rows(k), 1 - flip, k)
            if k > 0:
                total[...] = add_on(total[...], flip, k)

    proj = total[...]
    new_first = 0.8 * first[...] + 0.2 * proj
    new_second = 0.9 * second[...] + 0.1 * proj * proj
    fnew[...] = new_first
    snew[...] = new_second
    dirs[me] = (new_first / jnp.sqrt(new_second)).astype(BF16)
    def d_hop(way, j):
        origin = z + 1 - j if way == 0 else z - 1 + j
        view = dirs.at[2 * origin + y]
        target = z + 1 if way == 0 else z - 1
        return remote(view, view, d_send.at[way, j], d_recv.at[way, j], (2 * target + y, t))

    def d_in(way, j):
        origin = z - j if way == 0 else z + j
        view = dirs.at[2 * origin + y]
        return remote(view, view, d_send.at[way, j], d_recv.at[way, j], (me, t))

    def d_over(way, j):
        origin = z - j if way == 0 else z + j
        view = dirs.at[2 * origin + y]
        return remote(view, view, dy_send.at[way, j], dy_recv.at[way, j], (partner, t))

    def d_over_in(way, j):
        origin = z - j if way == 0 else z + j
        view = dirs.at[2 * origin + 1 - y]
        return remote(view, view, dy_send.at[way, j], dy_recv.at[way, j], (partner, t))

    def there(way, j):
        return z >= j if way == 0 else z < depth - j

    def more(way):
        return there(1 - way, 1)

    for way in (0, 1):
        pl.when(more(way))(d_hop(way, 1).start)
    d_over(0, 0).start()
    ticks('t')
    for j in range(1, depth):
        for way in (0, 1):
            @pl.when(there(way, j))
            def _():
                d_in(way, j).wait_recv()
                if j < depth - 1:
                    pl.when(more(way))(d_hop(way, j + 1).start)
                d_over(way, j).start()
        ticks(f'u{j}')

    ticks('v')
    d_over_in(0, 0).wait_recv()
    for j in range(1, depth):
        for way in (0, 1):
            pl.when(there(way, j))(d_over_in(way, j).wait_recv)
        ticks(f'v{j}')
    both = dirs[...].reshape(n * r, dirs.shape[2])
    squares = []
    for (upper, lower), part in zip(grams, (both[:, :gc], both[:, gc:])):
        lifted = jnp.dot(upper, part, preferred_element_type=F32)
        lifted = lifted + jnp.dot(lower, part, preferred_element_type=F32)
        squares.append(jnp.sum(part.astype(F32) * lifted))
    row = lax.broadcasted_iota(jnp.int32, sums.shape, 0)
    sums[...] = jnp.where(row == 0, squares[0], squares[1])
    s_copies = []
    for d in range(1, tp):
        c = remote(sums, sums_in.at[d], s_send.at[d], s_recv.at[d], (me, (t + d) % tp))
        c.start()
        s_copies.append(c)

    ticks('w')
    for c in s_copies:
        c.wait()
    whole = sums[...]
    for d in range(1, tp):
        whole = whole + sums_in[d]
    gscale = 0.02 / jnp.sqrt(whole[0:1, 0:1] / sizes[0] + 0.25)
    sscale = 0.02 / jnp.sqrt(whole[1:2, 0:1] / sizes[1] + 0.25)
    gdir, sdir = both[:, :gc], both[:, gc:]

    def updates(block, at):
        f = f_all[block, at, :]
        return (
            gscale * jnp.dot(f[:, :rank], gdir, preferred_element_type=F32),
            sscale * jnp.dot(f[:, rank:], sdir, preferred_element_type=F32),
        )

    def refresh(block, at):
        gstep, sstep = updates(block, at)
        wout[block, at, :gc] = (wg[block, at, :gc].astype(F32) - gstep).astype(BF16)
        wout[block, at, gc:] = (wg[block, at, gc:].astype(F32) - sstep).astype(BF16)

    every = pl.ds(0, rows)
    gstep, sstep = updates(me, every)
    wnew[:, :gc] = wide[:, :gc] - gstep
    wnew[:, gc:] = wide[:, gc:] - sstep
    wout[me] = wnew[...].astype(BF16)
    for s in range(1, steps):
        refresh(at_pos(pos - s), every)
        refresh(at_pos(pos + s), every)
    ticks('x')
    for h in range(parts):
        first_way = in_first(pos, h)
        if h < parts - 1:
            pl.when(first_way)(w_copies[0, steps - 1, h].wait_recv)
        if h > 0:
            pl.when(~first_way)(w_copies[1, steps - 1, h].wait_recv)
    refresh(at_pos(pos + steps), every)
    for (way, s, h), c in w_copies.items():
        pl.when(sent(way, s, h))(c.wait_send)
    for group in (f_copies, y_copies):
        for c in group.values():
            c.wait_send()
    for k in range(1, depth):
        pl.when(zz < k)(hop(flip, k, ahead).wait_send)
    for k in range(depth // 2 - 1):
        pl.when(zz > k)(hop(1 - flip, k, behind).wait_send)
    d_over(0, 0).wait_send()
    for way in (0, 1):
        for j in range(1, depth):
            pl.when(more(way) & there(way, j - 1))(d_hop(way, j).wait_send)
            pl.when(there(way, j))(d_over(way, j).wait_send)
    for trio in shares.values():
        for c in trio:
            c.wait_send()


def finish_kernel(wout, wnew, fnew, snew, gnew, snew_w, gcopy, scopy, gf_out, gs_out, sf_out, ss_out, sems):
    gc = gnew.shape[1]
    sc = snew_w.shape[1]
    n, rows, _ = wout.shape
    left, right = pl.ds(0, gc), pl.ds(gc, sc)
    pairs = []
    for b in range(n):
        at = pl.ds(b * rows, rows)
        pairs.append((wout.at[b, :, left], gcopy.at[at, :]))
        pairs.append((wout.at[b, :, right], scopy.at[at, :]))
    for src, gate, state in ((wnew, gnew, snew_w), (fnew, gf_out, sf_out), (snew, gs_out, ss_out)):
        pairs.append((src.at[:, left], gate))
        pairs.append((src.at[:, right], state))
    copies = [pltpu.make_async_copy(src, dst, sems.at[k]) for k, (src, dst) in enumerate(pairs)]
    for c in copies:
        c.start()
    for c in copies:
        c.wait()


def per_device(
    n, tp, inputs, gate_cot, state_cot, gate_weight, state_weight, gate_factor, state_factor,
    gate_first, gate_second, state_first, state_second,
):
    args = (
        inputs, gate_cot, state_cot, gate_weight, state_weight, gate_factor, state_factor,
        gate_first, gate_second, state_first, state_second,
    )
    tokens, d = inputs.shape
    rows, gc = gate_weight.shape
    sc = state_weight.shape[1]
    cols = gc + sc
    rank = gate_factor.shape[1]
    r = gate_first.shape[0]
    tiles = 3 if tokens % (3 * 128) == 0 else 1
    dma = pltpu.SemaphoreType.DMA
    anys = pl.BlockSpec(memory_space=pltpu.HBM)
    sds = jax.ShapeDtypeStruct
    steps = n // 2
    sizes = (n * rows * gc * tp, n * rows * sc * tp)
    held = pl.pallas_call(
        functools.partial(exchange_kernel, n, tp, tiles, sizes),
        out_shape=(
            pltpu.VMEM((n, rows, cols), BF16),
            pltpu.VMEM((rows, cols), F32),
            pltpu.VMEM((r, cols), F32),
            pltpu.VMEM((r, cols), F32),
        ),
        in_specs=[anys] * 11,
        out_specs=[pl.BlockSpec(memory_space=pltpu.VMEM)] * 4,
        scratch_shapes=[
            pltpu.VMEM((n, rows, cols), BF16),
            pltpu.VMEM((n, rows, 2 * rank), BF16),
            pltpu.VMEM((n, r, cols), BF16),
            pltpu.VMEM((tokens, d), BF16),
            pltpu.VMEM((tokens, gc), BF16),
            pltpu.VMEM((tokens, sc), BF16),
            pltpu.VMEM((rows, cols), F32),
            pltpu.VMEM((rows, cols), BF16),
            pltpu.VMEM((r, cols), F32),
            pltpu.VMEM((r, cols), F32),
            pltpu.VMEM((r, cols), F32),
            pltpu.VMEM((rank, cols), F32),
        ]
        + [pltpu.VMEM((steps, r, cols), BF16)] * 3
        + [pltpu.VMEM((2, steps, r, cols), BF16)]
        + [
            pltpu.VMEM((8, 128), F32),
            pltpu.VMEM((tp, 8, 128), F32),
            dma((11,)),
        ]
        + [dma((n,))] * 8
        + [dma((steps,))] * 3
        + [dma((2, steps))] * 5
        + [dma((tp,))] * 2
        + [dma((2, steps, 4))] * 2,
        compiler_params=pltpu.CompilerParams(
            collective_id=0, has_side_effects=True, vmem_limit_bytes=40 * 1024 * 1024
        ),
        name="exchange",
    )(*(pltpu.with_memory_space_constraint(a, pltpu.HBM) for a in args))

    outs = (gate_weight, state_weight, None, None, gate_first, gate_second, state_first, state_second)
    copies = (sds((n * rows, gc), BF16), sds((n * rows, sc), BF16))
    shapes = [sds(a.shape, a.dtype) for a in outs[:2]] + list(copies) + [sds(a.shape, a.dtype) for a in outs[4:]]
    return tuple(pl.pallas_call(
        finish_kernel,
        out_shape=tuple(shapes),
        in_specs=[pl.BlockSpec(memory_space=pltpu.VMEM)] * 4,
        out_specs=[anys] * 8,
        scratch_shapes=[dma((2 * n + 6,))],
        compiler_params=pltpu.CompilerParams(vmem_limit_bytes=4 * 1024 * 1024),
        name="finish",
    )(*(pltpu.with_memory_space_constraint(a, pltpu.VMEM) for a in held)))


def lifted_product(inputs, factor, cot):
    upper, lower = split(jnp.dot(inputs, factor, preferred_element_type=F32))
    first_part = jnp.einsum("tr,tc->rc", upper, cot, preferred_element_type=F32)
    return first_part + jnp.einsum("tr,tc->rc", lower, cot, preferred_element_type=F32)


def with_collectives(
    n, tp, inputs, gate_cot, state_cot, gate_weight, state_weight, gate_factor, state_factor,
    gate_first, gate_second, state_first, state_second,
):
    gc = gate_cot.shape[1]
    gate_part = lifted_product(inputs, lax.all_gather(gate_factor, "fs", axis=0, tiled=True), gate_cot)
    state_part = lifted_product(inputs, lax.all_gather(state_factor, "fs", axis=0, tiled=True), state_cot)
    partial_proj = jnp.concatenate([gate_part, state_part], 1)
    projection = lax.psum_scatter(partial_proj, "fs", scatter_dimension=0, tiled=True)
    first_new = 0.8 * jnp.concatenate([gate_first, state_first], 1) + 0.2 * projection
    second_new = 0.9 * jnp.concatenate([gate_second, state_second], 1) + 0.1 * projection * projection
    direction = (first_new / jnp.sqrt(second_new)).astype(BF16)
    dirs = lax.all_gather(direction, "fs", axis=0, tiled=True)
    gate_full = jnp.dot(gate_factor, dirs[:, :gc], preferred_element_type=F32)
    state_full = jnp.dot(state_factor, dirs[:, gc:], preferred_element_type=F32)
    gate_sq, state_sq = lax.psum(
        (jnp.sum(gate_full * gate_full), jnp.sum(state_full * state_full)), ("fs", "tp")
    )
    gate_scale = 0.02 / jnp.sqrt(gate_sq / (gate_full.size * n * tp) + 0.25)
    state_scale = 0.02 / jnp.sqrt(state_sq / (state_full.size * n * tp) + 0.25)
    gate_new = gate_weight - gate_scale * gate_full
    state_new = state_weight - state_scale * state_full
    gate_copy = lax.all_gather(gate_new.astype(BF16), "fs", axis=0, tiled=True)
    state_copy = lax.all_gather(state_new.astype(BF16), "fs", axis=0, tiled=True)
    return (
        gate_new, state_new, gate_copy, state_copy,
        first_new[:, :gc], second_new[:, :gc], first_new[:, gc:], second_new[:, gc:],
    )


def solution(mesh):
    n, tp = mesh.shape["fs"], mesh.shape["tp"]
    both = P("fs", "tp")
    wide = P("fs", None)

    def body(*args):
        r = args[7].shape[0]
        quarter = args[5].shape[0] // tp
        fits = tp == 4 and r % 16 == 0 and quarter % 16 == 0 and n >= 8
        return (per_device if fits else with_collectives)(n, tp, *args)

    return jax.shard_map(
        body,
        mesh=mesh,
        in_specs=(wide, both, both, both, both, wide, wide, both, both, both, both),
        out_specs=(both, both, P(None, "tp"), P(None, "tp"), both, both, both, both),
        check_vma=False,
    )
```

```python
import functools

import jax
import jax.numpy as jnp
from jax import lax
from jax.experimental import pallas as pl
from jax.experimental.pallas import tpu as pltpu
from jax.sharding import PartitionSpec as P

MESH = pl.DeviceIdType.MESH
BF16 = jnp.bfloat16
F32 = jnp.float32

KINDS = "omiy"
PLACE = {'a': ((0, 'omiy'), (1, 'miy'), (2, 'mi'), (3, 'mi')), 'c1': ((2, 'y'), (3, 'y'), (4, 'y'), (5, 'm')), 'd1': ((5, 'y'), (6, 'm')), 'r2': ((6, 'y'), (7, 'y'), (8, 'y'), (9, 'y')), 'r1': ((8, 'm'), (10, 'y')), 'v': ((11, 'y'),), 'v2': ((12, 'y'), (13, 'o'), (14, 'i')), 'w': ((13, 'my'), (14, 'omy'), (15, 'omy')), 'b3': ((1, 'o'), (2, 'o'), (3, 'o'), (4, 'm')), 'c2': ((4, 'o'), (5, 'o')), 'd3': ((6, 'o'),), 'q0': ((7, 'o'), (8, 'o')), 't': ((9, 'om'), (10, 'o'), (11, 'o'), (12, 'o')), 'b2': ((4, 'i'),), 'd5': ((5, 'i'),), 'd': ((6, 'i'),), 'g': ((7, 'i'), (8, 'i'), (9, 'i')), 's': ((10, 'i'),), 'u1': ((10, 'm'), (11, 'i')), 'u3': ((11, 'm'), (12, 'i'), (13, 'i')), 'v3': ((15, 'i'),), 'm0': ((7, 'm'),), 'v1': ((12, 'm'),)}


def over_rows(a, b):
    return lax.dot_general(a, b, (((0,), (0,)), ((), ())), preferred_element_type=F32)


def split(a):
    upper = a.astype(BF16)
    return upper, (a - upper.astype(F32)).astype(BF16)


def exchange_kernel(
    n, tp, tiles, sizes,
    x_hbm, gcot_hbm, scot_hbm, gw_hbm, sw_hbm, gf_hbm, sf_hbm, gfirst_hbm, gsecond_hbm, sfirst_hbm, ssecond_hbm,
    wout, wnew, fnew, snew,
    wg, f_all, dirs, x, gcot, scot, wide, wown, first, second, total, acc, send_y, recv_y, send_z, recv_z, sums, sums_in,
    load,
    f_send, f_recv, fx_send, fx_recv, fc_send, fc_recv, fd_send, fd_recv,
    ry_send, ry_recv, rz_send, rz_recv, d_send, d_recv, dy_send, dy_recv, s_send, s_recv, w_send, w_recv,
):
    me = lax.axis_index("fs")
    t = lax.axis_index("tp")
    rows, rank = gf_hbm.shape
    gc = gcot.shape[1]
    sc = scot.shape[1]
    r = first.shape[0]
    q = rows // tp
    depth = n // 2
    z, y = me // 2, me % 2
    partner = 2 * z + 1 - y

    sources = [
        (gf_hbm, f_all.at[me, :, pl.ds(0, rank)]),
        (sf_hbm, f_all.at[me, :, pl.ds(rank, rank)]),
        (gw_hbm, wide.at[:, pl.ds(0, gc)]),
        (sw_hbm, wide.at[:, pl.ds(gc, sc)]),
        (x_hbm, x),
        (gcot_hbm, gcot),
        (scot_hbm, scot),
        (gfirst_hbm, first.at[:, pl.ds(0, gc)]),
        (sfirst_hbm, first.at[:, pl.ds(gc, sc)]),
        (gsecond_hbm, second.at[:, pl.ds(0, gc)]),
        (ssecond_hbm, second.at[:, pl.ds(gc, sc)]),
    ]
    loads = [pltpu.make_async_copy(src, dst, load.at[k]) for k, (src, dst) in enumerate(sources)]
    for c in loads:
        c.start()

    def along_z(k):
        return 2 * ((z + depth + k) % depth) + y

    barrier = pltpu.get_barrier_semaphore()
    pl.semaphore_signal(barrier, inc=1, device_id=(partner, t), device_id_type=MESH)
    for k in range(1, depth):
        pl.semaphore_signal(barrier, inc=1, device_id=(along_z(k), t), device_id_type=MESH)
    for d in range(1, tp):
        pl.semaphore_signal(barrier, inc=1, device_id=(me, (t + d) % tp), device_id_type=MESH)
    pl.semaphore_wait(barrier, depth + tp - 1)

    def remote(src, dst, ss, rs, dev):
        return pltpu.make_async_remote_copy(
            src_ref=src, dst_ref=dst, send_sem=ss, recv_sem=rs, device_id=dev, device_id_type=MESH
        )

    core_peer = t + 1 - 2 * (t % 2)
    x_peer = (t + 2) % tp

    def source_block(j):
        k = j % depth
        return 2 * ((z + depth - k) % depth) + (y if j < depth else 1 - y)

    def quarter(block, which):
        return f_all.at[block, pl.ds(which * q, q), :]

    def first_leg(view, send, recv):
        copies = {}
        for j in sorted(range(1, depth), key=lambda k: -min(k, depth - k)) + [depth]:
            dev = partner if j == depth else along_z(j)
            copies[j] = remote(view(me), view(me), send.at[j], recv.at[j], (dev, t))
            copies[j].start()
        return copies

    def pass_over(copies, view, send, recv, k):
        b = source_block(k)
        copies[depth + k] = remote(
            view(b), view(b), send.at[depth + k], recv.at[depth + k], (partner, t)
        )
        copies[depth + k].start()

    loads[0].wait()
    loads[1].wait()
    mine = lambda b: quarter(b, t)
    f_copies = first_leg(mine, f_send, f_recv)

    loads[2].wait()
    loads[3].wait()
    wown[...] = wide[...].astype(BF16)

    pos = z + y * (n - 1 - 2 * z)

    def at_pos(p):
        p = (p + n) % n
        far = p // (n // 2)
        return 2 * p * (1 - far) + far * (2 * (n - 1 - p) + 1)

    right, left = at_pos(pos + 1), at_pos(pos - 1)
    steps = n // 2

    parts = 4
    piece = rows // parts

    def w_copy(way, s, h):
        block = at_pos(pos - s) if way == 0 else at_pos(pos + s)
        at = pl.ds(h * piece, piece)
        dst = wg.at[block, at, :]
        src = wown.at[at, :] if s == 0 else dst
        return remote(
            src, dst, w_send.at[way, s, h], w_recv.at[way, s, h], (right if way == 0 else left, t)
        )

    def in_first(p, h):
        p = (p + n) % n % steps
        share = parts // 2 - (p == 0).astype(jnp.int32) + (p == steps - 1).astype(jnp.int32)
        return h < share

    def sent(way, s, h):
        if s < steps - 1:
            return pos >= 0
        return in_first(pos + 1, h) if way == 0 else ~in_first(pos - 1, h)

    w_copies = {}

    spot = pos % steps

    def forward(way, s, k):
        h = k if way == 0 else parts - 1 - k
        if s > 0:
            w_copies[way, s - 1, h].wait_recv()
        if s < steps - 1:
            w_copies[way, s, h].start()
        elif k < parts - 1:
            pl.when(sent(way, s, h))(w_copies[way, s, h].start)

    def ticks(name):
        for i, kinds in PLACE.get(name, ()):
            s, k = i // parts, i % parts
            for way in (0, 1):
                h = k if way == 0 else parts - 1 - k
                if s < steps - 1 or k < parts - 1:
                    w_copies[way, s, h] = w_copy(way, s, h)
                if len(kinds) == len(KINDS):
                    forward(way, s, k)
                    continue
                for kind in kinds:
                    at = KINDS.index(kind)
                    at = at if way == 0 else steps - 1 - at
                    pl.when(spot == at)(functools.partial(forward, way, s, k))

    ticks('a')

    shares = {}

    def share(j):
        src = quarter(source_block(j), t)
        cx = remote(src, src, fx_send.at[j], fx_recv.at[j], (me, x_peer))
        cx.start()
        cc = remote(src, src, fc_send.at[j], fc_recv.at[j], (me, core_peer))
        cc.start()
        shares[j] = [cx, cc]

    order = sorted(range(1, depth), key=lambda k: min(k, depth - k))
    for k in order:
        f_copies[k].wait_recv()
        pass_over(f_copies, mine, f_send, f_recv, k)
        share(k)
        if k == order[0]:
            f_copies[depth].wait_recv()
            share(depth)
        ticks(f'b{k}')

    for k in order:
        f_copies[depth + k].wait_recv()
        share(depth + k)
        ticks(f'c{k}')
    for j, pair in shares.items():
        pair[0].wait_recv()
        src = quarter(source_block(j), x_peer)
        cd = remote(src, src, fd_send.at[j], fd_recv.at[j], (me, core_peer))
        cd.start()
        pair.append(cd)
        ticks(f'd{j}')
    for cx, cc, cd in shares.values():
        cc.wait_recv()
        cd.wait_recv()

    ticks('d')
    for k in (4, 5, 6):
        loads[k].wait()
    factor = f_all.reshape(n * rows, 2 * rank)
    step = x.shape[0] // tiles
    acc[...] = jnp.zeros_like(acc)

    for i in range(tiles):
        at = pl.ds(i * step, step)
        upper, lower = split(jnp.dot(x[at, :], factor[...], preferred_element_type=F32))
        g, s = gcot[at, :], scot[at, :]
        acc[:, :gc] += over_rows(upper[:, :rank], g) + over_rows(lower[:, :rank], g)
        acc[:, gc:] += over_rows(upper[:, rank:], s) + over_rows(lower[:, rank:], s)
        ticks(f'm{i}')

    def part_of(block):
        return acc[pl.ds(pl.multiple_of(block * r, r), r), :]

    low = z < depth // 2
    flip = 1 - low.astype(jnp.int32)
    zz = z + flip * (depth - 1 - 2 * z)
    ahead = z + 1 - 2 * flip
    behind = z - 1 + 2 * flip

    def level(k):
        return k + flip * (depth - 1 - 2 * k)

    y_copies = {}
    for k in reversed(range(depth)):
        send_y[k] = part_of(2 * level(k) + 1 - y).astype(BF16)
        y_copies[k] = remote(send_y.at[k], recv_y.at[k], ry_send.at[k], ry_recv.at[k], (partner, t))
        y_copies[k].start()
    ticks('e')

    grams = []
    for k in (0, 1):
        part = factor[:, k * rank:(k + 1) * rank]
        grams.append(split(over_rows(part, part)))

    ticks('g')
    def hop(way, k, target):
        goal = level(k)
        return remote(
            send_z.at[goal], recv_z.at[way, goal], rz_send.at[goal], rz_recv.at[way, goal],
            (2 * target + y, t),
        )

    def add_on(total, way, k):
        hop(way, k, z).wait_recv()
        return total + recv_z[way, level(k)].astype(F32)

    def both_rows(k):
        y_copies[k].wait_recv()
        return part_of(2 * level(k) + y) + recv_y[k].astype(F32)

    def pass_up(k):
        @pl.when(zz > 0)
        def _():
            send_z[level(k)] = add_on(both_rows(k), flip, k).astype(BF16)

        @pl.when(zz == 0)
        def _():
            send_z[level(k)] = both_rows(k).astype(BF16)

        hop(flip, k, ahead).start()

    for k in reversed(range(1, depth)):
        pl.when(zz < k)(functools.partial(pass_up, k))
        ticks(f'r{k}')
    for k in range(depth // 2 - 1):
        @pl.when(zz > k)
        def _():
            send_z[level(k)] = add_on(both_rows(k), 1 - flip, k).astype(BF16)
            hop(1 - flip, k, behind).start()
        ticks(f'q{k}')

    ticks('s')

    for c in loads[7:]:
        c.wait()
    for k in range(depth // 2):
        @pl.when(zz == k)
        def _():
            total[...] = add_on(both_rows(k), 1 - flip, k)
            if k > 0:
                total[...] = add_on(total[...], flip, k)

    proj = total[...]
    new_first = 0.8 * first[...] + 0.2 * proj
    new_second = 0.9 * second[...] + 0.1 * proj * proj
    fnew[...] = new_first
    snew[...] = new_second
    dirs[me] = (new_first / jnp.sqrt(new_second)).astype(BF16)
    def d_hop(way, j):
        origin = z + 1 - j if way == 0 else z - 1 + j
        view = dirs.at[2 * origin + y]
        target = z + 1 if way == 0 else z - 1
        return remote(view, view, d_send.at[way, j], d_recv.at[way, j], (2 * target + y, t))

    def d_in(way, j):
        origin = z - j if way == 0 else z + j
        view = dirs.at[2 * origin + y]
        return remote(view, view, d_send.at[way, j], d_recv.at[way, j], (me, t))

    def d_over(way, j):
        origin = z - j if way == 0 else z + j
        view = dirs.at[2 * origin + y]
        return remote(view, view, dy_send.at[way, j], dy_recv.at[way, j], (partner, t))

    def d_over_in(way, j):
        origin = z - j if way == 0 else z + j
        view = dirs.at[2 * origin + 1 - y]
        return remote(view, view, dy_send.at[way, j], dy_recv.at[way, j], (partner, t))

    def there(way, j):
        return z >= j if way == 0 else z < depth - j

    def more(way):
        return there(1 - way, 1)

    for way in (0, 1):
        pl.when(more(way))(d_hop(way, 1).start)
    d_over(0, 0).start()
    ticks('t')
    for j in range(1, depth):
        for way in (0, 1):
            @pl.when(there(way, j))
            def _():
                d_in(way, j).wait_recv()
                if j < depth - 1:
                    pl.when(more(way))(d_hop(way, j + 1).start)
                d_over(way, j).start()
        ticks(f'u{j}')

    ticks('v')
    d_over_in(0, 0).wait_recv()
    for j in range(1, depth):
        for way in (0, 1):
            pl.when(there(way, j))(d_over_in(way, j).wait_recv)
        ticks(f'v{j}')
    both = dirs[...].reshape(n * r, dirs.shape[2])
    squares = []
    for (upper, lower), part in zip(grams, (both[:, :gc], both[:, gc:])):
        lifted = jnp.dot(upper, part, preferred_element_type=F32)
        lifted = lifted + jnp.dot(lower, part, preferred_element_type=F32)
        squares.append(jnp.sum(part.astype(F32) * lifted))
    row = lax.broadcasted_iota(jnp.int32, sums.shape, 0)
    sums[...] = jnp.where(row == 0, squares[0], squares[1])
    s_copies = []
    for d in range(1, tp):
        c = remote(sums, sums_in.at[d], s_send.at[d], s_recv.at[d], (me, (t + d) % tp))
        c.start()
        s_copies.append(c)

    ticks('w')
    for c in s_copies:
        c.wait()
    whole = sums[...]
    for d in range(1, tp):
        whole = whole + sums_in[d]
    gscale = 0.02 / jnp.sqrt(whole[0:1, 0:1] / sizes[0] + 0.25)
    sscale = 0.02 / jnp.sqrt(whole[1:2, 0:1] / sizes[1] + 0.25)
    gdir, sdir = both[:, :gc], both[:, gc:]

    def updates(block, at):
        f = f_all[block, at, :]
        return (
            gscale * jnp.dot(f[:, :rank], gdir, preferred_element_type=F32),
            sscale * jnp.dot(f[:, rank:], sdir, preferred_element_type=F32),
        )

    def refresh(block, at):
        gstep, sstep = updates(block, at)
        wout[block, at, :gc] = (wg[block, at, :gc].astype(F32) - gstep).astype(BF16)
        wout[block, at, gc:] = (wg[block, at, gc:].astype(F32) - sstep).astype(BF16)

    every = pl.ds(0, rows)
    gstep, sstep = updates(me, every)
    wnew[:, :gc] = wide[:, :gc] - gstep
    wnew[:, gc:] = wide[:, gc:] - sstep
    wout[me] = wnew[...].astype(BF16)
    for s in range(1, steps):
        refresh(at_pos(pos - s), every)
        refresh(at_pos(pos + s), every)
    ticks('x')
    for h in range(parts):
        first_way = in_first(pos, h)
        if h < parts - 1:
            pl.when(first_way)(w_copies[0, steps - 1, h].wait_recv)
        if h > 0:
            pl.when(~first_way)(w_copies[1, steps - 1, h].wait_recv)
        if h % 2 == 1:
            refresh(at_pos(pos + steps), pl.ds((h - 1) * piece, 2 * piece))
    for (way, s, h), c in w_copies.items():
        pl.when(sent(way, s, h))(c.wait_send)
    for group in (f_copies, y_copies):
        for c in group.values():
            c.wait_send()
    for k in range(1, depth):
        pl.when(zz < k)(hop(flip, k, ahead).wait_send)
    for k in range(depth // 2 - 1):
        pl.when(zz > k)(hop(1 - flip, k, behind).wait_send)
    d_over(0, 0).wait_send()
    for way in (0, 1):
        for j in range(1, depth):
            pl.when(more(way) & there(way, j - 1))(d_hop(way, j).wait_send)
            pl.when(there(way, j))(d_over(way, j).wait_send)
    for trio in shares.values():
        for c in trio:
            c.wait_send()


def finish_kernel(wout, wnew, fnew, snew, gnew, snew_w, gcopy, scopy, gf_out, gs_out, sf_out, ss_out, sems):
    gc = gnew.shape[1]
    sc = snew_w.shape[1]
    n, rows, _ = wout.shape
    left, right = pl.ds(0, gc), pl.ds(gc, sc)
    pairs = []
    for b in range(n):
        at = pl.ds(b * rows, rows)
        pairs.append((wout.at[b, :, left], gcopy.at[at, :]))
        pairs.append((wout.at[b, :, right], scopy.at[at, :]))
    for src, gate, state in ((wnew, gnew, snew_w), (fnew, gf_out, sf_out), (snew, gs_out, ss_out)):
        pairs.append((src.at[:, left], gate))
        pairs.append((src.at[:, right], state))
    copies = [pltpu.make_async_copy(src, dst, sems.at[k]) for k, (src, dst) in enumerate(pairs)]
    for c in copies:
        c.start()
    for c in copies:
        c.wait()


def per_device(
    n, tp, inputs, gate_cot, state_cot, gate_weight, state_weight, gate_factor, state_factor,
    gate_first, gate_second, state_first, state_second,
):
    args = (
        inputs, gate_cot, state_cot, gate_weight, state_weight, gate_factor, state_factor,
        gate_first, gate_second, state_first, state_second,
    )
    tokens, d = inputs.shape
    rows, gc = gate_weight.shape
    sc = state_weight.shape[1]
    cols = gc + sc
    rank = gate_factor.shape[1]
    r = gate_first.shape[0]
    tiles = 3 if tokens % (3 * 128) == 0 else 1
    dma = pltpu.SemaphoreType.DMA
    anys = pl.BlockSpec(memory_space=pltpu.HBM)
    sds = jax.ShapeDtypeStruct
    steps = n // 2
    sizes = (n * rows * gc * tp, n * rows * sc * tp)
    held = pl.pallas_call(
        functools.partial(exchange_kernel, n, tp, tiles, sizes),
        out_shape=(
            pltpu.VMEM((n, rows, cols), BF16),
            pltpu.VMEM((rows, cols), F32),
            pltpu.VMEM((r, cols), F32),
            pltpu.VMEM((r, cols), F32),
        ),
        in_specs=[anys] * 11,
        out_specs=[pl.BlockSpec(memory_space=pltpu.VMEM)] * 4,
        scratch_shapes=[
            pltpu.VMEM((n, rows, cols), BF16),
            pltpu.VMEM((n, rows, 2 * rank), BF16),
            pltpu.VMEM((n, r, cols), BF16),
            pltpu.VMEM((tokens, d), BF16),
            pltpu.VMEM((tokens, gc), BF16),
            pltpu.VMEM((tokens, sc), BF16),
            pltpu.VMEM((rows, cols), F32),
            pltpu.VMEM((rows, cols), BF16),
            pltpu.VMEM((r, cols), F32),
            pltpu.VMEM((r, cols), F32),
            pltpu.VMEM((r, cols), F32),
            pltpu.VMEM((rank, cols), F32),
        ]
        + [pltpu.VMEM((steps, r, cols), BF16)] * 3
        + [pltpu.VMEM((2, steps, r, cols), BF16)]
        + [
            pltpu.VMEM((8, 128), F32),
            pltpu.VMEM((tp, 8, 128), F32),
            dma((11,)),
        ]
        + [dma((n,))] * 8
        + [dma((steps,))] * 3
        + [dma((2, steps))] * 5
        + [dma((tp,))] * 2
        + [dma((2, steps, 4))] * 2,
        compiler_params=pltpu.CompilerParams(
            collective_id=0, has_side_effects=True, vmem_limit_bytes=40 * 1024 * 1024
        ),
        name="exchange",
    )(*(pltpu.with_memory_space_constraint(a, pltpu.HBM) for a in args))

    outs = (gate_weight, state_weight, None, None, gate_first, gate_second, state_first, state_second)
    copies = (sds((n * rows, gc), BF16), sds((n * rows, sc), BF16))
    shapes = [sds(a.shape, a.dtype) for a in outs[:2]] + list(copies) + [sds(a.shape, a.dtype) for a in outs[4:]]
    return tuple(pl.pallas_call(
        finish_kernel,
        out_shape=tuple(shapes),
        in_specs=[pl.BlockSpec(memory_space=pltpu.VMEM)] * 4,
        out_specs=[anys] * 8,
        scratch_shapes=[dma((2 * n + 6,))],
        compiler_params=pltpu.CompilerParams(vmem_limit_bytes=4 * 1024 * 1024),
        name="finish",
    )(*(pltpu.with_memory_space_constraint(a, pltpu.VMEM) for a in held)))


def lifted_product(inputs, factor, cot):
    upper, lower = split(jnp.dot(inputs, factor, preferred_element_type=F32))
    first_part = jnp.einsum("tr,tc->rc", upper, cot, preferred_element_type=F32)
    return first_part + jnp.einsum("tr,tc->rc", lower, cot, preferred_element_type=F32)


def with_collectives(
    n, tp, inputs, gate_cot, state_cot, gate_weight, state_weight, gate_factor, state_factor,
    gate_first, gate_second, state_first, state_second,
):
    gc = gate_cot.shape[1]
    gate_part = lifted_product(inputs, lax.all_gather(gate_factor, "fs", axis=0, tiled=True), gate_cot)
    state_part = lifted_product(inputs, lax.all_gather(state_factor, "fs", axis=0, tiled=True), state_cot)
    partial_proj = jnp.concatenate([gate_part, state_part], 1)
    projection = lax.psum_scatter(partial_proj, "fs", scatter_dimension=0, tiled=True)
    first_new = 0.8 * jnp.concatenate([gate_first, state_first], 1) + 0.2 * projection
    second_new = 0.9 * jnp.concatenate([gate_second, state_second], 1) + 0.1 * projection * projection
    direction = (first_new / jnp.sqrt(second_new)).astype(BF16)
    dirs = lax.all_gather(direction, "fs", axis=0, tiled=True)
    gate_full = jnp.dot(gate_factor, dirs[:, :gc], preferred_element_type=F32)
    state_full = jnp.dot(state_factor, dirs[:, gc:], preferred_element_type=F32)
    gate_sq, state_sq = lax.psum(
        (jnp.sum(gate_full * gate_full), jnp.sum(state_full * state_full)), ("fs", "tp")
    )
    gate_scale = 0.02 / jnp.sqrt(gate_sq / (gate_full.size * n * tp) + 0.25)
    state_scale = 0.02 / jnp.sqrt(state_sq / (state_full.size * n * tp) + 0.25)
    gate_new = gate_weight - gate_scale * gate_full
    state_new = state_weight - state_scale * state_full
    gate_copy = lax.all_gather(gate_new.astype(BF16), "fs", axis=0, tiled=True)
    state_copy = lax.all_gather(state_new.astype(BF16), "fs", axis=0, tiled=True)
    return (
        gate_new, state_new, gate_copy, state_copy,
        first_new[:, :gc], second_new[:, :gc], first_new[:, gc:], second_new[:, gc:],
    )


def solution(mesh):
    n, tp = mesh.shape["fs"], mesh.shape["tp"]
    both = P("fs", "tp")
    wide = P("fs", None)

    def body(*args):
        r = args[7].shape[0]
        quarter = args[5].shape[0] // tp
        fits = tp == 4 and r % 16 == 0 and quarter % 16 == 0 and n >= 8
        return (per_device if fits else with_collectives)(n, tp, *args)

    return jax.shard_map(
        body,
        mesh=mesh,
        in_specs=(wide, both, both, both, both, wide, wide, both, both, both, both),
        out_specs=(both, both, P(None, "tp"), P(None, "tp"), both, both, both, both),
        check_vma=False,
    )
```
